32 devices in a mesh: sp: 16 (over z, y, x), tp: 2 (over core).
Axes of the slice: x: 2, y: 2, z: 4, core: 2. Of those that a mesh axis runs over, the one named last changes fastest.
Arguments:
- mixer_in: bfloat16 [8192, 1024], P('sp', 'tp'), may hold values from -6 to 6
- residual: bfloat16 [8192, 2048], P(('sp', 'tp')), may hold values from -6 to 6
- decay_real: float32 [64, 64], P('tp'), may hold values from -2 to 0, as said below
- decay_imag: float32 [64, 64], P('tp'), may hold values from 1 to 200
- log_step: float32 [64], P('tp'), may hold values from -3.9 to -2.5
- in_real: float32 [64, 64, 16], P('tp'), may hold values from -1 to 1
- in_imag: float32 [64, 64, 16], P('tp'), may hold values from -1 to 1
- output_real: float32 [64, 16, 64], P('tp'), may hold values from -0.5 to 0.5
- output_imaginary: float32 [64, 16, 64], P('tp'), may hold values from -0.5 to 0.5
- skip: float32 [1024], P('tp'), may hold values from -4 to 4
- out_proj: bfloat16 [1024, 2048], P('tp'), may hold values from -0.1875 to 0.1875
- norm_gain: float32 [2048], replicated, may hold values from 0.1 to 1.9
- w_gate: bfloat16 [2048, 5632], P('sp', 'tp'), may hold values from -0.125 to 0.125
- w_up: bfloat16 [2048, 5632], P('sp', 'tp'), may hold values from -0.125 to 0.125
- w_down: bfloat16 [5632, 2048], P('tp', 'sp'), may hold values from -0.078125 to 0.078125
Outputs:
- output: bfloat16 [8192, 2048], P(('sp', 'tp'))
The draws below stay inside these ranges and needn't reach their ends.
Inputs may be any that keep to these rules, and one draw needn't show every extreme that they name: `decay_real`: every entry is negative.
All inputs are finite; a program needn't handle non-finite values.
Results may differ from the reference program's by a relative error of at most 0.02.
Values may be sent and summed in bfloat16 or wider, within the bound.
No kernel may reach another device: no remote copies, remote signals or barrier semaphores. Data moves between devices by JAX's collectives and lax.ppermute only.
A program may use at most 128 MiB of HBM per device.

```python
import jax
import jax.numpy as jnp
from jax import lax

D = 2048
CH = 1024
GROUP = 16
STATE = 64
FF = 5632
TOK_DEV = 512
GROUPS = 64
TOKENS = 8192
CH_DEV = 512
FF_DEV = 2816
N_SP = 16


def draw_decay_real(key, part):
    slow_key, rate_key = jax.random.split(jax.random.fold_in(key, 11))
    slow = jax.random.bernoulli(slow_key, 0.5, (GROUPS, 1))
    mixing = jax.random.uniform(rate_key, (GROUPS, STATE), jnp.float32)
    slow_rate = 5.0 / TOKENS * jnp.exp(mixing * jnp.log(5.0))
    fast_rate = 0.6 * jnp.exp(mixing * jnp.log(2.0))
    return -jnp.where(slow, slow_rate, fast_rate)


def level_of(own_key, extent, shards, low, high):
    level = 1.0
    for position, parts in shards:
        heights = jax.random.uniform(jax.random.fold_in(jax.random.fold_in(own_key, 6), position), (parts,), jnp.float32, low / len(shards), high / len(shards))
        level = level * jnp.repeat(jnp.exp(heights), extent[position] // parts).reshape((-1,) + (1,) * (len(extent) - 1 - position))
    return level


def normal_values(key, shape, scale, bound, cuts=(), dtype=jnp.bfloat16):
    loudness = level_of(key, shape, cuts, -0.22, 0.18) if cuts else 1.0
    entries = jax.random.normal(key, shape, jnp.float32) * scale * loudness
    return jnp.minimum(jnp.maximum(entries, -bound), bound).astype(dtype)


def setup_inputs(seed: int = 0) -> dict:
    key_list = jax.random.split(jax.random.key(seed), 16)
    return {
        "mixer_in": normal_values(key_list[0], (TOKENS, CH), 1.0, 6.0, ((0, 16), (1, 2))),
        "residual": normal_values(key_list[1], (TOKENS, D), 1.0, 6.0, ((0, 32),)),
        "decay_real": draw_decay_real(jax.random.fold_in(key_list[15], 71), 0),
        "decay_imag": jnp.clip(1.0 + 199.0 * jax.random.uniform(key_list[3], (GROUPS, STATE), jnp.float32) ** level_of(key_list[3], (GROUPS, STATE), ((0, 2),), -0.2, 0.2), 1.0, 200.0),
        "log_step": jnp.clip(-3.9 + 1.4000001 * jax.random.uniform(key_list[4], (GROUPS,), jnp.float32) ** level_of(key_list[4], (GROUPS,), ((0, 2),), -0.2, 0.2), -3.9, -2.5),
        "in_real": normal_values(key_list[5], (GROUPS, STATE, GROUP), (2 * GROUP) ** -0.5, 1.0, ((0, 2),), jnp.float32),
        "in_imag": normal_values(key_list[6], (GROUPS, STATE, GROUP), (2 * GROUP) ** -0.5, 1.0, ((0, 2),), jnp.float32),
        "output_real": normal_values(key_list[7], (GROUPS, GROUP, STATE), (2 * STATE) ** -0.5, 0.5, ((0, 2),), jnp.float32),
        "output_imaginary": normal_values(key_list[8], (GROUPS, GROUP, STATE), (2 * STATE) ** -0.5, 0.5, ((0, 2),), jnp.float32),
        "skip": normal_values(key_list[9], (CH,), 1.0, 4.0, ((0, 2),), jnp.float32),
        "out_proj": normal_values(key_list[10], (CH, D), CH ** -0.5, 0.1875, ((0, 2),)),
        "norm_gain": jnp.clip(1.0 + 0.18 * jax.random.normal(key_list[11], (D,), jnp.float32), 0.1, 1.9),
        "w_gate": normal_values(key_list[12], (D, FF), D ** -0.5, 0.125, ((0, 16), (1, 2))),
        "w_up": normal_values(key_list[13], (D, FF), D ** -0.5, 0.125, ((0, 16), (1, 2))),
        "w_down": normal_values(key_list[14], (FF, D), FF ** -0.5, 0.078125, ((0, 2), (1, 16))),
    }


def discrete(decay_real, decay_imag, log_step, in_real, in_imag):
    step_size = jnp.exp(log_step)[:, None]
    magnitude = jnp.exp(decay_real * step_size)
    angle = decay_imag * step_size
    power_re = magnitude * jnp.cos(angle)
    power_im = magnitude * jnp.sin(angle)
    denom = decay_real * decay_real + decay_imag * decay_imag
    ratio_re = ((power_re - 1.0) * decay_real + power_im * decay_imag) / denom
    ratio_im = (power_im * decay_real - (power_re - 1.0) * decay_imag) / denom
    drive_re = ratio_re[..., None] * in_real - ratio_im[..., None] * in_imag
    drive_im = ratio_re[..., None] * in_imag + ratio_im[..., None] * in_real
    return (power_re, power_im, drive_re, drive_im)

def combine(earlier, later):
    ar1, ai1, br1, bi1 = earlier
    ar2, ai2, br2, bi2 = later
    return (ar2 * ar1 - ai2 * ai1, ar2 * ai1 + ai2 * ar1, ar2 * br1 - ai2 * bi1 + br2, ar2 * bi1 + ai2 * br1 + bi2)

def block_sum(left, right, width):
    summed = jnp.zeros((left.shape[0], right.shape[1]), jnp.float32)
    for index in range(left.shape[1] // width):
        partial_value = jnp.dot(left[:, index * width:(index + 1) * width], right[index * width:(index + 1) * width], preferred_element_type=jnp.float32).astype(jnp.bfloat16)
        summed = summed + lax.optimization_barrier(partial_value).astype(jnp.float32)
    return summed.astype(jnp.bfloat16)

def reference(mixer_in, residual, decay_real, decay_imag, log_step, in_real, in_imag, output_real, output_imaginary, skip, out_proj, norm_gain, w_gate, w_up, w_down):
    highest_precision = lax.Precision.HIGHEST
    power_re, power_im, bar_re, bar_im = discrete(decay_real, decay_imag, log_step, in_real, in_imag)
    groups, states = decay_real.shape
    signal = mixer_in.astype(jnp.float32).reshape(N_SP, TOK_DEV, groups, GROUP)
    group_skip_gain = skip.reshape(groups, GROUP)

    def advance(carry, block_range):
        hold_re, hold_im = carry
        drive_re = jnp.einsum('tgc,gpc->tgp', block_range, bar_re, precision=highest_precision)
        drive_im = jnp.einsum('tgc,gpc->tgp', block_range, bar_im, precision=highest_precision)
        a_re = jnp.broadcast_to(power_re[None], drive_re.shape)
        a_im = jnp.broadcast_to(power_im[None], drive_re.shape)
        pw_re, pw_im, state_real, state_imaginary = lax.associative_scan(combine, (a_re, a_im, drive_re, drive_im), axis=0)
        state_real = state_real + pw_re * hold_re[None] - pw_im * hold_im[None]
        state_imaginary = state_imaginary + pw_re * hold_im[None] + pw_im * hold_re[None]
        mixed_before_norm = jnp.einsum('uzl,zhl->uzh', state_real, output_real, precision=highest_precision) - jnp.einsum('uzl,zhl->uzh', state_imaginary, output_imaginary, precision=highest_precision) + group_skip_gain[None] * block_range
        return ((state_real[-1], state_imaginary[-1]), mixed_before_norm.reshape(TOK_DEV, groups * GROUP))
    zero_state = jnp.zeros((groups, states), jnp.float32)
    _, mixed_all = lax.scan(advance, (zero_state, zero_state), signal)
    activated = jax.nn.gelu(mixed_all).astype(jnp.bfloat16)
    res_blocks = residual.reshape(N_SP, TOK_DEV, residual.shape[1])

    def finish(pair):
        act_rows, res_rows = pair
        mixed = block_sum(act_rows, out_proj, CH_DEV)
        carried = res_rows.astype(jnp.float32) + mixed.astype(jnp.float32)
        scale = lax.rsqrt(lax.optimization_barrier(jnp.mean(carried * carried, axis=-1, keepdims=True)) + 1e-06)
        normed = (carried * scale * norm_gain).astype(jnp.bfloat16)
        gate = jnp.dot(normed, w_gate, preferred_element_type=jnp.float32)
        up = jnp.dot(normed, w_up, preferred_element_type=jnp.float32)
        hidden = (jax.nn.silu(gate) * up).astype(jnp.bfloat16)
        down = block_sum(hidden, w_down, FF_DEV)
        return (carried + 0.5 * down.astype(jnp.float32)).astype(jnp.bfloat16)
    result = lax.map(finish, (activated, res_blocks))
    return result.reshape(TOKENS, residual.shape[1])
```

```python
import jax
import jax.numpy as jnp
from jax import lax
from jax.sharding import PartitionSpec as P


def before_mine(decay_re, decay_im, last_re, last_im):
    count = lax.axis_size("sp")

    def shift(value, distance):
        return lax.ppermute(value, "sp", [(i, i + distance) for i in range(count - distance)])

    hold = shift(jnp.stack([last_re, last_im]), 1)
    distance = 1
    while distance < count:
        moved = shift(hold, distance)
        hold = hold + jnp.stack(
            [
                decay_re * moved[0] - decay_im * moved[1],
                decay_re * moved[1] + decay_im * moved[0],
            ]
        )
        decay_re, decay_im = (
            decay_re * decay_re - decay_im * decay_im,
            2.0 * decay_re * decay_im,
        )
        distance = distance * 2
    return (hold[0], hold[1])


def discrete(decay_real, decay_imag, log_step, in_real, in_imag):
    step_size = jnp.exp(log_step)[:, None]
    magnitude = jnp.exp(decay_real * step_size)
    angle = decay_imag * step_size
    power_re = magnitude * jnp.cos(angle)
    power_im = magnitude * jnp.sin(angle)
    denom = decay_real * decay_real + decay_imag * decay_imag
    ratio_re = ((power_re - 1.0) * decay_real + power_im * decay_imag) / denom
    ratio_im = (power_im * decay_real - (power_re - 1.0) * decay_imag) / denom
    drive_re = ratio_re[..., None] * in_real - ratio_im[..., None] * in_imag
    drive_im = ratio_re[..., None] * in_imag + ratio_im[..., None] * in_real
    return (power_re, power_im, drive_re, drive_im)


def combine(earlier, later):
    ar1, ai1, br1, bi1 = earlier
    ar2, ai2, br2, bi2 = later
    return (
        ar2 * ar1 - ai2 * ai1,
        ar2 * ai1 + ai2 * ar1,
        ar2 * br1 - ai2 * bi1 + br2,
        ar2 * bi1 + ai2 * br1 + bi2,
    )


def spread_blocks(matrix):
    groups = matrix.shape[0]
    unit_blocks = jnp.eye(groups, dtype=jnp.float32)[:, None, :, None]
    turned = jnp.transpose(matrix, (0, 2, 1))[:, :, None, :]
    return (unit_blocks * turned).reshape(groups * matrix.shape[2], groups * matrix.shape[1])


def local_states(power_re, power_im, drive_re, drive_im):
    rows, flat_size = drive_re.shape
    span = 8
    blocks = rows // span
    dr = drive_re.reshape(blocks, span, flat_size)
    di = drive_im.reshape(blocks, span, flat_size)
    cur_re = dr[:, 0]
    cur_im = di[:, 0]
    inner_re = [cur_re]
    inner_im = [cur_im]
    lift_re = [power_re]
    lift_im = [power_im]
    for index in range(1, span):
        cur_re, cur_im = (
            power_re * cur_re - power_im * cur_im + dr[:, index],
            power_re * cur_im + power_im * cur_re + di[:, index],
        )
        inner_re.append(cur_re)
        inner_im.append(cur_im)
        prev_re, prev_im = (lift_re[-1], lift_im[-1])
        lift_re.append(power_re * prev_re - power_im * prev_im)
        lift_im.append(power_re * prev_im + power_im * prev_re)
    inner_re = jnp.stack(inner_re, axis=1)
    inner_im = jnp.stack(inner_im, axis=1)
    lift_re = jnp.concatenate(lift_re, axis=0)[None]
    lift_im = jnp.concatenate(lift_im, axis=0)[None]
    block_re = jnp.broadcast_to(lift_re[0, span - 1][None], (blocks, flat_size))
    block_im = jnp.broadcast_to(lift_im[0, span - 1][None], (blocks, flat_size))
    totals = (block_re, block_im, cur_re, cur_im)
    distance = 1
    while distance < blocks:
        ones = jnp.ones((distance, flat_size), jnp.float32)
        zeros = jnp.zeros((distance, flat_size), jnp.float32)
        moved = (
            jnp.concatenate([ones, totals[0][:-distance]], axis=0),
            jnp.concatenate([zeros, totals[1][:-distance]], axis=0),
            jnp.concatenate([zeros, totals[2][:-distance]], axis=0),
            jnp.concatenate([zeros, totals[3][:-distance]], axis=0),
        )
        totals = combine(moved, totals)
        distance = distance * 2
    one_row = jnp.ones((1, flat_size), jnp.float32)
    zero_row = jnp.zeros((1, flat_size), jnp.float32)
    hold_re, hold_im = before_mine(
        totals[0][-1], totals[1][-1], totals[2][-1], totals[3][-1]
    )
    before_a_re = jnp.concatenate([one_row, totals[0][:-1]], axis=0)
    before_a_im = jnp.concatenate([zero_row, totals[1][:-1]], axis=0)
    before_re = jnp.concatenate([zero_row, totals[2][:-1]], axis=0)
    before_im = jnp.concatenate([zero_row, totals[3][:-1]], axis=0)
    before_re, before_im = (
        (before_re + before_a_re * hold_re - before_a_im * hold_im)[:, None],
        (before_im + before_a_re * hold_im + before_a_im * hold_re)[:, None],
    )
    state_real = inner_re + lift_re * before_re - lift_im * before_im
    state_imaginary = inner_im + lift_re * before_im + lift_im * before_re
    return (state_real.reshape(rows, flat_size), state_imaginary.reshape(rows, flat_size))


def swap(value, axis):
    count = lax.axis_size(axis)
    return lax.ppermute(value, axis, [(i, i ^ 1) for i in range(count)])


def half_of(value, which, dim):
    size = value.shape[dim] // 2
    return lax.dynamic_slice_in_dim(value, which * size, size, axis=dim)


def add_halves(one, two):
    return (one.astype(jnp.float32) + two.astype(jnp.float32)).astype(jnp.bfloat16)


def share_rows(rows):
    if lax.axis_size("tp") == 2:
        return jnp.concatenate([rows, swap(rows, "tp")], axis=0)
    return lax.all_gather(rows, "tp", axis=0, tiled=True)


def return_rows(partial_value):
    if lax.axis_size("tp") == 2:
        size = partial_value.shape[0] // 2
        return add_halves(partial_value[:size], swap(partial_value[size:], "tp"))
    return lax.psum_scatter(partial_value, "tp", scatter_dimension=0, tiled=True)


def pair_weights(weight, side, split_dim, join_dim):
    kept = half_of(weight, side, split_dim)
    got = swap(half_of(weight, 1 - side, split_dim), "sp")
    lower = jnp.where(side == 0, kept, got)
    upper = jnp.where(side == 0, got, kept)
    return jnp.concatenate([lower, upper], axis=join_dim)


def on_device(
    mixer_in,
    residual,
    decay_real,
    decay_imag,
    log_step,
    in_real,
    in_imag,
    output_real,
    output_imaginary,
    skip,
    out_proj,
    norm_gain,
    w_gate,
    w_up,
    w_down,
):
    power_re, power_im, bar_re, bar_im = discrete(
        decay_real, decay_imag, log_step, in_real, in_imag
    )
    count = lax.axis_size("sp")
    side = lax.axis_index("sp") % 2
    same_side = [list(range(first, count, 2)) for first in range(2)]
    gate_up = jnp.concatenate(
        [pair_weights(w_gate, side, 1, 0), pair_weights(w_up, side, 1, 0)], axis=1
    )
    gate_up = lax.all_gather(gate_up, "sp", axis=0, tiled=True, axis_index_groups=same_side)
    down_columns = lax.all_gather(
        pair_weights(w_down, side, 0, 1), "sp", axis=0, axis_index_groups=same_side
    )

    groups, states = decay_real.shape
    flat_size = groups * states
    span = 8 if groups % 8 == 0 else groups
    high = lax.Precision.HIGH
    signal = mixer_in.astype(jnp.float32)
    width = span * in_real.shape[2]
    drive_re = []
    drive_im = []
    for block in range(groups // span):
        part = slice(block * span, (block + 1) * span)
        piece = signal[:, block * width : (block + 1) * width]
        drive_re.append(jnp.dot(piece, spread_blocks(bar_re[part]), precision=high))
        drive_im.append(jnp.dot(piece, spread_blocks(bar_im[part]), precision=high))
    state_real, state_imaginary = local_states(
        power_re.reshape(1, flat_size),
        power_im.reshape(1, flat_size),
        jnp.concatenate(drive_re, axis=1),
        jnp.concatenate(drive_im, axis=1),
    )
    mixed_before_norm = []
    for block in range(groups // span):
        part = slice(block * span, (block + 1) * span)
        lanes = slice(block * span * states, (block + 1) * span * states)
        mixed_before_norm.append(
            jnp.dot(state_real[:, lanes], spread_blocks(output_real[part]), precision=high)
            - jnp.dot(
                state_imaginary[:, lanes], spread_blocks(output_imaginary[part]), precision=high
            )
        )
    mixed_before_norm = jnp.concatenate(mixed_before_norm, axis=1) + skip[None] * signal
    activated = jax.nn.gelu(mixed_before_norm).astype(jnp.bfloat16)
    partial_value = jnp.dot(activated, out_proj, preferred_element_type=jnp.float32).astype(
        jnp.bfloat16
    )
    if lax.axis_size("tp") == 2:
        core = lax.axis_index("tp")
        mixed = add_halves(
            half_of(partial_value, core, 0), swap(half_of(partial_value, 1 - core, 0), "tp")
        )
    else:
        mixed = lax.psum_scatter(partial_value, "tp", scatter_dimension=0, tiled=True)
    carried = residual.astype(jnp.float32) + mixed.astype(jnp.float32)
    scale = lax.rsqrt(jnp.mean(carried * carried, axis=-1, keepdims=True) + 1e-06)
    normed = (carried * scale * norm_gain).astype(jnp.bfloat16)
    own_rows = share_rows(normed)
    pair_rows = share_rows(swap(normed, "sp"))
    units = gate_up.shape[1] // 2

    def feed(rows):
        both = jnp.dot(rows, gate_up, preferred_element_type=jnp.float32)
        return (jax.nn.silu(both[:, :units]) * both[:, units:]).astype(jnp.bfloat16)

    def lower(hidden):
        columns = [
            jnp.dot(hidden, down_columns[i], preferred_element_type=jnp.float32).astype(
                jnp.bfloat16
            )
            for i in range(down_columns.shape[0])
        ]
        return return_rows(jnp.concatenate(columns, axis=1))

    own_hidden = feed(own_rows)
    theirs = swap(lower(feed(pair_rows)), "sp")
    down = add_halves(lower(own_hidden), theirs)
    return (carried + 0.5 * down.astype(jnp.float32)).astype(jnp.bfloat16)


def solution(mesh):
    return jax.shard_map(
        on_device,
        mesh=mesh,
        in_specs=(
            P("sp", "tp"),
            P(("sp", "tp"), None),
            P("tp", None),
            P("tp", None),
            P("tp"),
            P("tp", None, None),
            P("tp", None, None),
            P("tp", None, None),
            P("tp", None, None),
            P("tp"),
            P("tp", None),
            P(),
            P("sp", "tp"),
            P("sp", "tp"),
            P("tp", "sp"),
        ),
        out_specs=P(("sp", "tp"), None),
        check_vma=False,
    )
```
